32 devices in a mesh: ra: 4 (over z), cb: 2 (over y), dp: 4 (over x, core).
Axes of the slice: x: 2, y: 2, z: 4, core: 2. Of those that a mesh axis runs over, the one named last changes fastest.
Arguments:
- stream: bfloat16 [1024, 2048], P('dp', 'ra'), may hold values from -60 to 60
- norm_gain: float32 [2, 2048], P(None, 'ra'), may hold values from 0.1 to 1.9
- gate_weight: float32 [2, 2048, 5504], P(None, 'ra', 'cb'), may hold values from -0.125 to 0.125
- up_weight: float32 [2, 2048, 5504], P(None, 'ra', 'cb'), may hold values from -0.125 to 0.125
- down_weight: float32 [2, 5504, 2048], P(None, 'cb', 'ra'), may hold values from -0.078125 to 0.078125
- gate_scale: float32 [2, 5504], P(None, 'cb'), may hold values from 0.5 to 2
- up_scale: float32 [2, 5504], P(None, 'cb'), may hold values from 0.5 to 2
- down_scale: float32 [2, 2048], P(None, 'ra'), may hold values from 0.5 to 2
Outputs:
- result: bfloat16 [1024, 2048], P('dp', 'ra')
The draws below stay inside these ranges and needn't reach their ends.
All inputs are finite; a program needn't handle non-finite values.
Results may differ from the reference program's by a relative error of at most 0.04.
Values may be sent and summed in bfloat16 or wider, within the bound.
A program may use at most 128 MiB of HBM per device.

```python
import math
import jax
import jax.numpy as jnp
from jax import lax

D = 2048
FF = 5504
TOKENS = 1024
N_RA = 4


def draw_stream(key, part):
    keys = jax.random.split(jax.random.fold_in(key, 11), 3)
    position = jnp.arange(D).astype(jnp.float32) / D
    column_scale = 0.3 * 10.0 ** position * jax.random.uniform(keys[0], (D,), jnp.float32, 0.7, 1.4)
    row_scale = 10.0 ** jax.random.uniform(keys[1], (TOKENS, 1), jnp.float32, -0.5, 0.5)
    base = jnp.clip(jax.random.normal(keys[2], (TOKENS, D), jnp.float32), -4.0, 4.0)
    return (base * row_scale * column_scale).astype(jnp.bfloat16)


def level_of(key, dims, cuts, low, largest):
    level = 1.0
    for dim, blocks in cuts:
        heights = jax.random.uniform(jax.random.fold_in(jax.random.fold_in(key, 6), dim), (blocks,), jnp.float32, low / len(cuts), largest / len(cuts))
        level = level * jnp.repeat(jnp.exp(heights), dims[dim] // blocks).reshape((-1,) + (1,) * (len(dims) - 1 - dim))
    return level


def centred(rng, shape, scale, reach, shards=(), dtype=jnp.bfloat16):
    loudness = level_of(rng, shape, shards, -0.22, 0.18) if shards else 1.0
    drawn = jax.random.normal(rng, shape, jnp.float32) * scale * loudness
    return jnp.minimum(jnp.maximum(drawn, -reach), reach).astype(dtype)


def setup_inputs(seed: int = 0) -> dict:
    splits = jax.random.split(jax.random.key(seed), 9)
    stream = draw_stream(jax.random.fold_in(splits[8], 71), 0)
    norm_gain = jnp.clip(1.0 + 0.18 * jax.random.normal(splits[1], (2, D), jnp.float32), 0.1, 1.9)
    gate_weight = centred(splits[2], (2, D, FF), D ** -0.5, 0.125, ((1, 4), (2, 2)), jnp.float32)
    up_weight = centred(splits[3], (2, D, FF), D ** -0.5, 0.125, ((1, 4), (2, 2)), jnp.float32)
    down_weight = centred(splits[4], (2, FF, D), FF ** -0.5, 0.078125, ((1, 2), (2, 4)), jnp.float32)
    gate_scale = jnp.clip(jnp.exp(math.log(2.0) - 1.3862944 * jax.random.uniform(splits[5], (2, FF), jnp.float32) ** level_of(splits[5], (2, FF), ((1, 2),), -0.2, 0.2)), 0.5, 2.0)
    up_scale = jnp.clip(jnp.exp(math.log(2.0) - 1.3862944 * jax.random.uniform(splits[6], (2, FF), jnp.float32) ** level_of(splits[6], (2, FF), ((1, 2),), -0.2, 0.2)), 0.5, 2.0)
    down_scale = jnp.clip(jnp.exp(math.log(2.0) - 1.3862944 * jax.random.uniform(splits[7], (2, D), jnp.float32) ** level_of(splits[7], (2, D), ((1, 4),), -0.2, 0.2)), 0.5, 2.0)
    return {"stream": stream, "norm_gain": norm_gain, "gate_weight": gate_weight, "up_weight": up_weight, "down_weight": down_weight, "gate_scale": gate_scale, "up_scale": up_scale, "down_scale": down_scale}


epsilon = 1e-06
residual_scale = 0.5

def block_sums(normed, weight):
    width = D // N_RA

    def add_block(carry, index):
        start = (index * width).astype(jnp.int32)
        columns = lax.dynamic_slice_in_dim(normed, start, width, 1)
        rows = lax.dynamic_slice_in_dim(weight, start, width, 0)
        piece = jnp.dot(columns, rows, preferred_element_type=jnp.float32).astype(jnp.bfloat16)
        piece = lax.optimization_barrier(piece)
        return (carry + piece.astype(jnp.float32), None)
    initial = jnp.zeros((normed.shape[0], weight.shape[1]), jnp.float32)
    total, unused = lax.scan(add_block, initial, jnp.arange(N_RA).astype(jnp.int32))
    return total

def half_step(stream, gain, gate_weight, up_weight, down_weight, gate_scale, up_scale, down_scale):
    widened = stream.astype(jnp.float32)
    squares = lax.optimization_barrier(jnp.sum(widened * widened, axis=1, keepdims=True))
    inverse = lax.rsqrt(squares / D + epsilon)
    normed = (widened * gain).astype(jnp.bfloat16)
    gate_sum = block_sums(normed, gate_weight.astype(jnp.bfloat16)) * inverse * gate_scale
    up_sum = block_sums(normed, up_weight.astype(jnp.bfloat16)) * inverse * up_scale
    hidden = (jax.nn.silu(gate_sum) * up_sum).astype(jnp.bfloat16)
    branch = jnp.dot(hidden, down_weight.astype(jnp.bfloat16), preferred_element_type=jnp.float32) * down_scale
    return (residual_scale * widened + branch).astype(jnp.bfloat16)

def reference(stream, norm_gain, gate_weight, up_weight, down_weight, gate_scale, up_scale, down_scale):
    current = stream
    for block_index in range(2):
        current = half_step(current, norm_gain[block_index], gate_weight[block_index], up_weight[block_index], down_weight[block_index], gate_scale[block_index], up_scale[block_index], down_scale[block_index])
    return current
```

```python
import functools

import jax
import jax.numpy as jnp
from jax import lax
from jax.experimental import pallas as pl
from jax.experimental.pallas import tpu as pltpu
from jax.sharding import PartitionSpec as P

MESH = pl.DeviceIdType.MESH
epsilon = 1e-06
residual_scale = 0.5
WIDTH = 128
TILE = 256
LAG = 2
SUBLANES = 8


def kernel(
    n, m, stream, gain, gate_hbm, up_hbm, down_hbm, gate_scale, up_scale, down_scale, out,
    gate_v, up_v, down_v, part, sums_in, hidden, sq, sq_in, inverse, scales, normed, acc, y_buf, current,
    w_sem, rs_send, rs_recv, ag_send, ag_recv, sq_send, sq_recv, y_send, y_recv,
):
    blocks = gate_hbm.shape[0]
    units = gate_hbm.shape[2]
    rows, depth = stream.shape
    half = rows // 2
    features = depth * n
    chunks = pl.cdiv(units, WIDTH)
    r = lax.axis_index("ra")
    q = lax.axis_index("cb")
    first, final = r == 0, r == n - 1
    left, right = jnp.maximum(r - 1, 0), jnp.minimum(r + 1, n - 1)
    head, last = (final, first), (first, final)
    onward, back = (left, right), (right, left)
    passed = (n - 1 - r, r)

    def weight_copies(b):
        return [
            pltpu.make_async_copy(hbm.at[b], vmem.at[b], w_sem.at[b, i])
            for i, (hbm, vmem) in enumerate(
                ((gate_hbm, gate_v), (up_hbm, up_v), (down_hbm, down_v))
            )
        ]

    loads = [weight_copies(b) for b in range(blocks)]
    loads[0][0].start()
    loads[0][1].start()

    barrier = pltpu.get_barrier_semaphore()

    for i in range(1, n):
        peer = lax.rem(r + i, n)
        pl.semaphore_signal(barrier, inc=1, device_id={"ra": peer}, device_id_type=MESH)

    for i in range(1, m):
        peer = lax.rem(q + i, m)
        pl.semaphore_signal(barrier, inc=1, device_id={"cb": peer}, device_id_type=MESH)

    def sum_copy(b, d, c):
        return pltpu.make_async_remote_copy(
            src_ref=part.at[b, c, d], dst_ref=sums_in.at[b, c, d],
            send_sem=rs_send.at[b, d, c], recv_sem=rs_recv.at[b, d, c],
            device_id={"ra": onward[d]}, device_id_type=MESH,
        )

    def hidden_copy(b, d, c):
        piece = hidden.at[b, c, pl.ds(d * half, half)]
        return pltpu.make_async_remote_copy(
            src_ref=piece, dst_ref=piece,
            send_sem=ag_send.at[b, d, c], recv_sem=ag_recv.at[b, d, c],
            device_id={"ra": back[d]}, device_id_type=MESH,
        )

    def squares_copy(b, d, source):
        return pltpu.make_async_remote_copy(
            src_ref=sq.at[b, d], dst_ref=sq_in.at[b, d, source],
            send_sem=sq_send.at[b, d], recv_sem=sq_recv.at[b, d, source],
            device_id={"ra": (n - 1) * d}, device_id_type=MESH,
        )

    def branch_copy(b, i):
        return pltpu.make_async_remote_copy(
            src_ref=y_buf.at[b, q], dst_ref=y_buf.at[b, q],
            send_sem=y_send.at[b, i - 1], recv_sem=y_recv.at[b, q],
            device_id={"cb": lax.rem(q + i, m)}, device_id_type=MESH,
        )

    def branch_arrival(b, i):
        source = lax.rem(q + i, m)
        return pltpu.make_async_remote_copy(
            src_ref=y_buf.at[b, source], dst_ref=y_buf.at[b, source],
            send_sem=y_send.at[b, i - 1], recv_sem=y_recv.at[b, source],
            device_id={"cb": source}, device_id_type=MESH,
        )

    current[...] = stream[...]
    for c in range(chunks):
        lo = c * WIDTH
        w = min(WIDTH, units - lo)
        for b in range(blocks):
            for g, scale in enumerate((gate_scale, up_scale)):
                scales[g, b, c, :, :w] = scale[b : b + 1, lo : lo + w]

    for b in range(blocks):
        widened = current[...].astype(jnp.float32)
        normed[...] = (widened * gain[b : b + 1, :]).astype(jnp.bfloat16)
        squares = jnp.sum(widened * widened, axis=1, keepdims=True)
        for d in range(2):
            column = squares[d * half : (d + 1) * half]
            sq[b, d] = jnp.broadcast_to(column, (half, WIDTH)).T[:SUBLANES]

        if b == 0:
            pl.semaphore_wait(barrier, n - 1 + m - 1)

        for d in range(2):
            @pl.when(jnp.logical_not(last[d]))
            def _(d=d):
                squares_copy(b, d, r).start()

        loads[b][0].wait()
        loads[b][1].wait()
        if b == 0:
            loads[0][2].start()
            for later in range(1, blocks):
                for load in loads[later]:
                    load.start()

        for lo in range(0, units, TILE):
            w = min(TILE, units - lo)
            cuts = [(at, min(WIDTH, w - at)) for at in range(0, w, WIDTH)]
            for g, weight in enumerate((gate_v, up_v)):
                piece = jnp.dot(
                    normed[...], weight[b, :, lo : lo + w].astype(jnp.bfloat16),
                    preferred_element_type=jnp.float32,
                ).astype(jnp.bfloat16)
                for d in range(2):
                    for at, cut in cuts:
                        part[b, (lo + at) // WIDTH, d, g, :, :cut] = piece[
                            d * half : (d + 1) * half, at : at + cut
                        ]
            for d in range(2):
                @pl.when(head[d])
                def _(d=d, lo=lo, cuts=cuts):
                    for at, cut in cuts:
                        sum_copy(b, d, (lo + at) // WIDTH).start()

        loads[b][2].wait()
        acc[...] = jnp.zeros_like(acc)
        pairs = units // TILE

        def step(t, carry, b=b):
            for d in range(2):
                c = t - (passed[d] - 1) * LAG
                live = (passed[d] > 0) & (c >= 0) & (c < chunks)

                @pl.when(live & jnp.logical_not(last[d]))
                def _(d=d, c=c):
                    sum_copy(b, d, c).wait_recv()
                    part[b, c, d] = (
                        part[b, c, d].astype(jnp.float32) + sums_in[b, c, d].astype(jnp.float32)
                    ).astype(jnp.bfloat16)
                    sum_copy(b, d, c).start()

                @pl.when(live & last[d] & (c == 0))
                def _(d=d):
                    total = sq[b, d]
                    for i in range(1, n):
                        source = lax.rem(r + i, n)
                        squares_copy(b, d, source).wait_recv()
                        total = total + sq_in[b, d, source]
                    column = jnp.broadcast_to(total[:1], (WIDTH, half)).T
                    inverse[b, d] = lax.rsqrt(column / features + epsilon)

                @pl.when(live & last[d])
                def _(d=d, c=c):
                    sum_copy(b, d, c).wait_recv()
                    gate_sum, up_sum = (
                        (
                            part[b, c, d, g].astype(jnp.float32)
                            + sums_in[b, c, d, g].astype(jnp.float32)
                        )
                        * inverse[b, d]
                        * scales[g, b, c]
                        for g in range(2)
                    )
                    active = gate_sum / (1.0 + jnp.exp(-gate_sum)) * up_sum
                    hidden[b, c, d * half : (d + 1) * half, :] = active.astype(jnp.bfloat16)
                    hidden_copy(b, d, c).start()

            for d in range(2):
                far = n - 1 - passed[d]
                c = t - (n - 2 + far) * LAG
                live = (far > 0) & (c >= 0) & (c < chunks)

                @pl.when(live)
                def _(d=d, c=c):
                    hidden_copy(b, d, c).wait_recv()

                @pl.when(live & jnp.logical_not(head[d]))
                def _(d=d, c=c):
                    hidden_copy(b, d, c).start()

            c = t - (2 * n - 3) * LAG

            @pl.when((c >= 0) & (lax.rem(c, 2) == 1) & (c < 2 * pairs))
            def _():
                both = jnp.concatenate([hidden[b, c - 1], hidden[b, c]], axis=1)
                at = pl.multiple_of((c - 1) * WIDTH, TILE)
                acc[...] += jnp.dot(
                    both, down_v[b, pl.ds(at, TILE), :].astype(jnp.bfloat16),
                    preferred_element_type=jnp.float32,
                )

            return carry

        lax.fori_loop(0, chunks + (2 * n - 3) * LAG, step, 0)
        for c in range(2 * pairs, chunks):
            lo = c * WIDTH
            w = min(WIDTH, units - lo)
            acc[...] += jnp.dot(
                hidden[b, c, :, :w], down_v[b, lo : lo + w, :].astype(jnp.bfloat16),
                preferred_element_type=jnp.float32,
            )

        y_buf[b, q] = acc[...].astype(jnp.bfloat16)
        for i in range(1, m):
            branch_copy(b, i).start()
        for i in range(1, m):
            branch_arrival(b, i).wait_recv()
        branch = y_buf[b, 0].astype(jnp.float32)
        for j in range(1, m):
            branch = branch + y_buf[b, j].astype(jnp.float32)
        branch = branch * down_scale[b : b + 1, :]
        result = (residual_scale * current[...].astype(jnp.float32) + branch).astype(jnp.bfloat16)
        if b == blocks - 1:
            out[...] = result
        else:
            current[...] = result

    for b in range(blocks):
        for i in range(1, m):
            branch_copy(b, i).wait_send()
        for d in range(2):
            @pl.when(jnp.logical_not(last[d]))
            def _(d=d, b=b):
                squares_copy(b, d, r).wait_send()

                @pl.loop(0, chunks)
                def _(c):
                    sum_copy(b, d, c).wait_send()

            @pl.when(jnp.logical_not(head[d]))
            def _(d=d, b=b):
                @pl.loop(0, chunks)
                def _(c):
                    hidden_copy(b, d, c).wait_send()


def on_device(n, m, stream, norm_gain, gate_weight, up_weight, down_weight, gate_scale, up_scale, down_scale):
    rows, depth = stream.shape
    half = rows // 2
    blocks, _, units = gate_weight.shape
    chunks = pl.cdiv(units, WIDTH)
    vmem = pl.BlockSpec(memory_space=pltpu.VMEM)
    whole = pl.BlockSpec(memory_space=pl.ANY)
    dma = pltpu.SemaphoreType.DMA
    return pl.pallas_call(
        functools.partial(kernel, n, m),
        out_shape=jax.ShapeDtypeStruct(stream.shape, jnp.bfloat16),
        in_specs=[vmem, vmem, whole, whole, whole, vmem, vmem, vmem],
        out_specs=vmem,
        scratch_shapes=[
            pltpu.VMEM(gate_weight.shape, jnp.float32),
            pltpu.VMEM(up_weight.shape, jnp.float32),
            pltpu.VMEM(down_weight.shape, jnp.float32),
            pltpu.VMEM((blocks, chunks, 2, 2, half, WIDTH), jnp.bfloat16),
            pltpu.VMEM((blocks, chunks, 2, 2, half, WIDTH), jnp.bfloat16),
            pltpu.VMEM((blocks, chunks, rows, WIDTH), jnp.bfloat16),
            pltpu.VMEM((blocks, 2, SUBLANES, half), jnp.float32),
            pltpu.VMEM((blocks, 2, n, SUBLANES, half), jnp.float32),
            pltpu.VMEM((blocks, 2, half, WIDTH), jnp.float32),
            pltpu.VMEM((2, blocks, chunks, 1, WIDTH), jnp.float32),
            pltpu.VMEM((rows, depth), jnp.bfloat16),
            pltpu.VMEM((rows, depth), jnp.float32),
            pltpu.VMEM((blocks, m, rows, depth), jnp.bfloat16),
            pltpu.VMEM((rows, depth), jnp.bfloat16),
            dma((blocks, 3)),
            dma((blocks, 2, chunks)),
            dma((blocks, 2, chunks)),
            dma((blocks, 2, chunks)),
            dma((blocks, 2, chunks)),
            dma((blocks, 2)),
            dma((blocks, 2, n)),
            dma((blocks, m)),
            dma((blocks, m)),
        ],
        compiler_params=pltpu.CompilerParams(
            collective_id=0, has_side_effects=True, vmem_limit_bytes=67043328
        ),
    )(stream, norm_gain, gate_weight, up_weight, down_weight, gate_scale, up_scale, down_scale)


def solution(mesh):
    in_specs = (
        P("dp", "ra"),
        P(None, "ra"),
        P(None, "ra", "cb"),
        P(None, "ra", "cb"),
        P(None, "cb", "ra"),
        P(None, "cb"),
        P(None, "cb"),
        P(None, "ra"),
    )
    return jax.shard_map(
        functools.partial(on_device, mesh.shape["ra"], mesh.shape["cb"]),
        mesh=mesh, in_specs=in_specs, out_specs=P("dp", "ra"), check_vma=False,
    )
```

```python
import functools

import jax
import jax.numpy as jnp
from jax import lax
from jax.experimental import pallas as pl
from jax.experimental.pallas import tpu as pltpu
from jax.sharding import PartitionSpec as P

MESH = pl.DeviceIdType.MESH
epsilon = 1e-06
residual_scale = 0.5
WIDTH = 128
TILE = 256
AHEAD = 4
LAG = 2
SUBLANES = 8


def kernel(
    n, m, stream, gain, gate_hbm, up_hbm, down_hbm, gate_scale, up_scale, down_scale, out,
    gate_v, up_v, down_v, part, sums_in, hidden, sq, sq_in, inverse, scales, normed, acc, y_buf, current,
    w_sem, rs_send, rs_recv, ag_send, ag_recv, sq_send, sq_recv, y_send, y_recv,
):
    blocks = gate_hbm.shape[0]
    units = gate_hbm.shape[2]
    rows, depth = stream.shape
    half = rows // 2
    features = depth * n
    chunks = pl.cdiv(units, WIDTH)
    r = lax.axis_index("ra")
    q = lax.axis_index("cb")
    first, final = r == 0, r == n - 1
    left, right = jnp.maximum(r - 1, 0), jnp.minimum(r + 1, n - 1)
    head, last = (final, first), (first, final)
    onward, back = (left, right), (right, left)
    passed = (n - 1 - r, r)

    def weight_copies(b):
        return [
            pltpu.make_async_copy(hbm.at[b], vmem.at[b], w_sem.at[b, i])
            for i, (hbm, vmem) in enumerate(
                ((gate_hbm, gate_v), (up_hbm, up_v), (down_hbm, down_v))
            )
        ]

    loads = [weight_copies(b) for b in range(blocks)]
    loads[0][0].start()
    loads[0][1].start()

    barrier = pltpu.get_barrier_semaphore()

    for i in range(1, n):
        peer = lax.rem(r + i, n)
        pl.semaphore_signal(barrier, inc=1, device_id={"ra": peer}, device_id_type=MESH)

    for i in range(1, m):
        peer = lax.rem(q + i, m)
        pl.semaphore_signal(barrier, inc=1, device_id={"cb": peer}, device_id_type=MESH)

    def sum_copy(b, d, c):
        return pltpu.make_async_remote_copy(
            src_ref=part.at[b, c, d], dst_ref=sums_in.at[b, c, d],
            send_sem=rs_send.at[b, d, c], recv_sem=rs_recv.at[b, d, c],
            device_id={"ra": onward[d]}, device_id_type=MESH,
        )

    def hidden_copy(b, d, c):
        piece = hidden.at[b, c, pl.ds(d * half, half)]
        return pltpu.make_async_remote_copy(
            src_ref=piece, dst_ref=piece,
            send_sem=ag_send.at[b, d, c], recv_sem=ag_recv.at[b, d, c],
            device_id={"ra": back[d]}, device_id_type=MESH,
        )

    def squares_copy(b, d, source):
        return pltpu.make_async_remote_copy(
            src_ref=sq.at[b, d], dst_ref=sq_in.at[b, d, source],
            send_sem=sq_send.at[b, d], recv_sem=sq_recv.at[b, d, source],
            device_id={"ra": (n - 1) * d}, device_id_type=MESH,
        )

    def branch_copy(b, i):
        return pltpu.make_async_remote_copy(
            src_ref=y_buf.at[b, q], dst_ref=y_buf.at[b, q],
            send_sem=y_send.at[b, i - 1], recv_sem=y_recv.at[b, q],
            device_id={"cb": lax.rem(q + i, m)}, device_id_type=MESH,
        )

    def branch_arrival(b, i):
        source = lax.rem(q + i, m)
        return pltpu.make_async_remote_copy(
            src_ref=y_buf.at[b, source], dst_ref=y_buf.at[b, source],
            send_sem=y_send.at[b, i - 1], recv_sem=y_recv.at[b, source],
            device_id={"cb": source}, device_id_type=MESH,
        )

    current[...] = stream[...]
    for c in range(chunks):
        lo = c * WIDTH
        w = min(WIDTH, units - lo)
        for b in range(blocks):
            for g, scale in enumerate((gate_scale, up_scale)):
                scales[g, b, c, :, :w] = scale[b : b + 1, lo : lo + w]

    for b in range(blocks):
        widened = current[...].astype(jnp.float32)
        normed[...] = (widened * gain[b : b + 1, :]).astype(jnp.bfloat16)
        squares = jnp.sum(widened * widened, axis=1, keepdims=True)
        for d in range(2):
            column = squares[d * half : (d + 1) * half]
            sq[b, d] = jnp.broadcast_to(column, (half, WIDTH)).T[:SUBLANES]

        if b == 0:
            pl.semaphore_wait(barrier, n - 1 + m - 1)

        for d in range(2):
            @pl.when(jnp.logical_not(last[d]))
            def _(d=d):
                squares_copy(b, d, r).start()

        loads[b][0].wait()
        loads[b][1].wait()
        if b == 0:
            loads[0][2].start()
            for later in range(1, blocks):
                for load in loads[later]:
                    load.start()

        for lo in range(0, units, TILE):
            w = min(TILE, units - lo)
            cuts = [(at, min(WIDTH, w - at)) for at in range(0, w, WIDTH)]
            for g, weight in enumerate((gate_v, up_v)):
                piece = jnp.dot(
                    normed[...], weight[b, :, lo : lo + w].astype(jnp.bfloat16),
                    preferred_element_type=jnp.float32,
                ).astype(jnp.bfloat16)
                for d in range(2):
                    for at, cut in cuts:
                        part[b, (lo + at) // WIDTH, d, g, :, :cut] = piece[
                            d * half : (d + 1) * half, at : at + cut
                        ]
            for d in range(2):
                @pl.when(head[d])
                def _(d=d, lo=lo, cuts=cuts):
                    for at, cut in cuts:
                        if (lo + at) // WIDTH < AHEAD:
                            sum_copy(b, d, (lo + at) // WIDTH).start()

        loads[b][2].wait()
        acc[...] = jnp.zeros_like(acc)
        pairs = units // TILE

        def step(t, carry, b=b):
            for d in range(2):
                @pl.when(head[d] & (t + AHEAD < chunks))
                def _(d=d):
                    sum_copy(b, d, t + AHEAD).start()

            for d in range(2):
                c = t - (passed[d] - 1) * LAG
                live = (passed[d] > 0) & (c >= 0) & (c < chunks)

                @pl.when(live & jnp.logical_not(last[d]))
                def _(d=d, c=c):
                    sum_copy(b, d, c).wait_recv()
                    part[b, c, d] = (
                        part[b, c, d].astype(jnp.float32) + sums_in[b, c, d].astype(jnp.float32)
                    ).astype(jnp.bfloat16)
                    sum_copy(b, d, c).start()

                @pl.when(live & last[d] & (c == 0))
                def _(d=d):
                    total = sq[b, d]
                    for i in range(1, n):
                        source = lax.rem(r + i, n)
                        squares_copy(b, d, source).wait_recv()
                        total = total + sq_in[b, d, source]
                    column = jnp.broadcast_to(total[:1], (WIDTH, half)).T
                    inverse[b, d] = lax.rsqrt(column / features + epsilon)

                @pl.when(live & last[d])
                def _(d=d, c=c):
                    sum_copy(b, d, c).wait_recv()
                    gate_sum, up_sum = (
                        (
                            part[b, c, d, g].astype(jnp.float32)
                            + sums_in[b, c, d, g].astype(jnp.float32)
                        )
                        * inverse[b, d]
                        * scales[g, b, c]
                        for g in range(2)
                    )
                    active = gate_sum / (1.0 + jnp.exp(-gate_sum)) * up_sum
                    hidden[b, c, d * half : (d + 1) * half, :] = active.astype(jnp.bfloat16)
                    hidden_copy(b, d, c).start()

            for d in range(2):
                far = n - 1 - passed[d]
                c = t - (n - 2 + far) * LAG
                live = (far > 0) & (c >= 0) & (c < chunks)

                @pl.when(live)
                def _(d=d, c=c):
                    hidden_copy(b, d, c).wait_recv()

                @pl.when(live & jnp.logical_not(head[d]))
                def _(d=d, c=c):
                    hidden_copy(b, d, c).start()

            c = t - (2 * n - 3) * LAG

            @pl.when((c >= 0) & (lax.rem(c, 2) == 1) & (c < 2 * pairs))
            def _():
                both = jnp.concatenate([hidden[b, c - 1], hidden[b, c]], axis=1)
                at = pl.multiple_of((c - 1) * WIDTH, TILE)
                acc[...] += jnp.dot(
                    both, down_v[b, pl.ds(at, TILE), :].astype(jnp.bfloat16),
                    preferred_element_type=jnp.float32,
                )

            return carry

        lax.fori_loop(0, chunks + (2 * n - 3) * LAG, step, 0)
        for c in range(2 * pairs, chunks):
            lo = c * WIDTH
            w = min(WIDTH, units - lo)
            acc[...] += jnp.dot(
                hidden[b, c, :, :w], down_v[b, lo : lo + w, :].astype(jnp.bfloat16),
                preferred_element_type=jnp.float32,
            )

        y_buf[b, q] = acc[...].astype(jnp.bfloat16)
        for i in range(1, m):
            branch_copy(b, i).start()
        for i in range(1, m):
            branch_arrival(b, i).wait_recv()
        branch = y_buf[b, 0].astype(jnp.float32)
        for j in range(1, m):
            branch = branch + y_buf[b, j].astype(jnp.float32)
        branch = branch * down_scale[b : b + 1, :]
        result = (residual_scale * current[...].astype(jnp.float32) + branch).astype(jnp.bfloat16)
        if b == blocks - 1:
            out[...] = result
        else:
            current[...] = result

    for b in range(blocks):
        for i in range(1, m):
            branch_copy(b, i).wait_send()
        for d in range(2):
            @pl.when(jnp.logical_not(last[d]))
            def _(d=d, b=b):
                squares_copy(b, d, r).wait_send()

                @pl.loop(0, chunks)
                def _(c):
                    sum_copy(b, d, c).wait_send()

            @pl.when(jnp.logical_not(head[d]))
            def _(d=d, b=b):
                @pl.loop(0, chunks)
                def _(c):
                    hidden_copy(b, d, c).wait_send()


def on_device(n, m, stream, norm_gain, gate_weight, up_weight, down_weight, gate_scale, up_scale, down_scale):
    rows, depth = stream.shape
    half = rows // 2
    blocks, _, units = gate_weight.shape
    chunks = pl.cdiv(units, WIDTH)
    vmem = pl.BlockSpec(memory_space=pltpu.VMEM)
    whole = pl.BlockSpec(memory_space=pl.ANY)
    dma = pltpu.SemaphoreType.DMA
    return pl.pallas_call(
        functools.partial(kernel, n, m),
        out_shape=jax.ShapeDtypeStruct(stream.shape, jnp.bfloat16),
        in_specs=[vmem, vmem, whole, whole, whole, vmem, vmem, vmem],
        out_specs=vmem,
        scratch_shapes=[
            pltpu.VMEM(gate_weight.shape, jnp.float32),
            pltpu.VMEM(up_weight.shape, jnp.float32),
            pltpu.VMEM(down_weight.shape, jnp.float32),
            pltpu.VMEM((blocks, chunks, 2, 2, half, WIDTH), jnp.bfloat16),
            pltpu.VMEM((blocks, chunks, 2, 2, half, WIDTH), jnp.bfloat16),
            pltpu.VMEM((blocks, chunks, rows, WIDTH), jnp.bfloat16),
            pltpu.VMEM((blocks, 2, SUBLANES, half), jnp.float32),
            pltpu.VMEM((blocks, 2, n, SUBLANES, half), jnp.float32),
            pltpu.VMEM((blocks, 2, half, WIDTH), jnp.float32),
            pltpu.VMEM((2, blocks, chunks, 1, WIDTH), jnp.float32),
            pltpu.VMEM((rows, depth), jnp.bfloat16),
            pltpu.VMEM((rows, depth), jnp.float32),
            pltpu.VMEM((blocks, m, rows, depth), jnp.bfloat16),
            pltpu.VMEM((rows, depth), jnp.bfloat16),
            dma((blocks, 3)),
            dma((blocks, 2, chunks)),
            dma((blocks, 2, chunks)),
            dma((blocks, 2, chunks)),
            dma((blocks, 2, chunks)),
            dma((blocks, 2)),
            dma((blocks, 2, n)),
            dma((blocks, m)),
            dma((blocks, m)),
        ],
        compiler_params=pltpu.CompilerParams(
            collective_id=0, has_side_effects=True, vmem_limit_bytes=67043328
        ),
    )(stream, norm_gain, gate_weight, up_weight, down_weight, gate_scale, up_scale, down_scale)


def solution(mesh):
    in_specs = (
        P("dp", "ra"),
        P(None, "ra"),
        P(None, "ra", "cb"),
        P(None, "ra", "cb"),
        P(None, "cb", "ra"),
        P(None, "cb"),
        P(None, "cb"),
        P(None, "ra"),
    )
    return jax.shard_map(
        functools.partial(on_device, mesh.shape["ra"], mesh.shape["cb"]),
        mesh=mesh, in_specs=in_specs, out_specs=P("dp", "ra"), check_vma=False,
    )
```
